32 devices in a mesh: grp: 2 (over y), sp: 4 (over z), tp: 4 (over x, core).
Axes of the slice: x: 2, y: 2, z: 4, core: 2. Of those that a mesh axis runs over, the one named last changes fastest.
Arguments:
- starting_stream: bfloat16 [3072, 2048], P(('grp', 'sp'), 'tp'), parts along dimension 0, may hold values from -45 to 45
- multiplier_matrix: bfloat16 [2, 2048, 2048], P(None, 'sp', 'tp'), may hold values from -0.125 to 0.125
- memory_path_matrix: bfloat16 [2, 2048, 2048], P(None, 'sp', 'tp'), may hold values from -0.125 to 0.125
- filter_coefficients: bfloat16 [2, 4, 2048], P(None, None, 'tp'), may hold values from -3 to 3
- memory_valve_matrix: bfloat16 [2, 8, 256, 256], P(None, 'tp'), may hold values from -0.375 to 0.375
- entry_valve_matrix: bfloat16 [2, 8, 256, 256], P(None, 'tp'), may hold values from -0.375 to 0.375
- forgetting_parameters: float32 [2, 2048], P(None, 'tp'), may hold values from 3 to 15
- timestep_forgetting_multiplier: float32 [3072], P(('grp', 'sp')), parts along dimension 0, may hold values from 0.5 to 2
- spike_extra: float32 [3072, 2048], P(('grp', 'sp'), 'tp'), parts along dimension 0, may hold values from -0.7 to 0
- exit_projector_matrix: bfloat16 [2, 2048, 2048], P(None, 'tp', 'sp'), may hold values from -0.125 to 0.125
- prelude_rms_gains: float32 [2, 2048], replicated, may hold values from 0.1 to 1.9
- finishing_rms_gains: float32 [2048], P('tp'), may hold values from 0.1 to 1.9
Outputs:
- result: bfloat16 [3072, 2048], P(('grp', 'sp'), 'tp'), parts along dimension 0
The draws below stay inside these ranges and needn't reach their ends.
There are 2 independent parts, one for each index of `grp`. The reference program is written for one: setup_inputs(seed, part) draws one part's arguments, and reference() takes and returns one part's arrays. A program takes and returns all parts, laid end to end along the dimension named above; an argument that names none is the same for every part. Nothing has to cross between parts.
All inputs are finite; a program needn't handle non-finite values.
Results may differ from the reference program's by a relative error of at most 0.015.
Values may be sent and summed in bfloat16 or wider, within the bound.
A program may use at most 64 MiB of HBM per device.

```python
import math
import jax
import jax.numpy as jnp
from jax import lax

D = 2048
W = 2048
BLOCK_W = 256
BLOCKS = 8
CONV = 4
LAYERS = 2
TOK_DEV = 384
TOKENS = 1536
N_TP = 4


def draw_starting_stream(key, part):
    keys = jax.random.split(key, 3)
    columns = jnp.arange(D, dtype=jnp.float32)
    col_scale = jnp.exp(math.log(4.0) * columns / D) * jax.random.uniform(keys[1], (D,), jnp.float32, 0.7, 1.4)
    row_scale = jnp.exp(jax.random.uniform(keys[2], (TOKENS, 1), jnp.float32, math.log(0.5), math.log(2.0)))
    base = jnp.clip(jax.random.normal(keys[0], (TOKENS, D), jnp.float32), -4.0, 4.0)
    return (base * col_scale[None, :] * row_scale).astype(jnp.bfloat16)


def draw_forgetting_parameters(key, part):
    keys = jax.random.split(key, 3)
    share_fast = 0.5
    fast = jax.random.bernoulli(keys[0], share_fast, (LAYERS, W))
    fast_rate = jnp.exp(jax.random.uniform(keys[1], (LAYERS, W), jnp.float32, math.log(0.01), math.log(0.03)))
    slow_rate = jnp.exp(jax.random.uniform(keys[2], (LAYERS, W), jnp.float32, math.log(0.1), math.log(0.5))) / (4.0 * TOKENS)
    rate = jnp.where(fast, fast_rate, slow_rate)
    return -jnp.log(jnp.expm1(rate))


def draw_timestep_forgetting_multiplier(key, part):
    counted = TOKENS // TOK_DEV
    values = jnp.exp(jax.random.uniform(key, (counted,), jnp.float32, math.log(0.5), math.log(2.0)))
    return jnp.repeat(values, TOK_DEV, total_repeat_length=TOKENS)


def draw_spike_extra(key, part):
    keys = jax.random.split(key, 2)
    spots = jax.random.randint(keys[0], (4,), 0, TOKENS)
    places = jnp.arange(TOKENS, dtype=jnp.int32)
    struck = jnp.any(places[:, None] == spots[None, :], axis=1)
    depth = jnp.log(jax.random.uniform(keys[1], (TOKENS, W), jnp.float32, 0.5, 0.8))
    return jnp.where(struck[:, None], depth, 0.0)


def levels(own_key, dims, shards, least, high):
    factor_of, own = 1.0, jax.random.fold_in(own_key, 6)
    for axis_at, shards_of in shards:
        draws = jnp.exp(jax.random.uniform(jax.random.fold_in(own, axis_at), (shards_of,), jnp.float32, least / len(shards), high / len(shards)))
        factor_of = factor_of * jnp.repeat(draws, dims[axis_at] // shards_of).reshape([-1 if axis == axis_at else 1 for axis in range(len(dims))])
    return factor_of


def gaussian(stream_key, shape, scale, reach, shards=(), held_as=jnp.bfloat16):
    level = levels(stream_key, shape, shards, -0.22, 0.18) if shards else 1.0
    array = jax.random.normal(stream_key, shape, jnp.float32) * scale * level
    return jnp.minimum(jnp.maximum(array, -reach), reach).astype(held_as)


def setup_inputs(seed: int = 0, part: int = 0) -> dict:
    seeds = jax.random.split(jax.random.key(seed), 13)
    part_keys = jax.random.split(jax.random.fold_in(seeds[12], part), 13)
    return {
        "starting_stream": draw_starting_stream(jax.random.fold_in(jax.random.fold_in(seeds[12], part), 71), part),
        "multiplier_matrix": gaussian(seeds[1], (LAYERS, D, W), D ** -0.5, 0.125, ((1, 4), (2, 4))),
        "memory_path_matrix": gaussian(seeds[2], (LAYERS, D, W), D ** -0.5, 0.125, ((1, 4), (2, 4))),
        "filter_coefficients": gaussian(seeds[3], (LAYERS, CONV, W), CONV ** -0.5, 3.0, ((2, 4),)),
        "memory_valve_matrix": gaussian(seeds[4], (LAYERS, BLOCKS, BLOCK_W, BLOCK_W), BLOCK_W ** -0.5, 0.375, ((1, 4),)),
        "entry_valve_matrix": gaussian(seeds[5], (LAYERS, BLOCKS, BLOCK_W, BLOCK_W), BLOCK_W ** -0.5, 0.375, ((1, 4),)),
        "forgetting_parameters": draw_forgetting_parameters(jax.random.fold_in(seeds[12], 71), part),
        "timestep_forgetting_multiplier": draw_timestep_forgetting_multiplier(jax.random.fold_in(jax.random.fold_in(seeds[12], part), 71), part),
        "spike_extra": draw_spike_extra(jax.random.fold_in(jax.random.fold_in(seeds[12], part), 71), part),
        "exit_projector_matrix": gaussian(seeds[9], (LAYERS, W, D), W ** -0.5, 0.125, ((1, 4), (2, 4))),
        "prelude_rms_gains": jnp.clip(1.0 + 0.18 * jax.random.normal(seeds[10], (LAYERS, D), jnp.float32), 0.1, 1.9),
        "finishing_rms_gains": jnp.clip(1.0 + 0.18 * jax.random.normal(seeds[11], (D,), jnp.float32), 0.1, 1.9),
    }


EPSILON = 1e-06
SQUASH_POWER = 8.0

def norm_rows(values, gain):
    mean_square = lax.optimization_barrier(jnp.mean(values * values, axis=-1, keepdims=True))
    return values * lax.rsqrt(mean_square + EPSILON) * gain

def combine_pairs(earlier, later):
    return (earlier[0] * later[0], later[0] * earlier[1] + later[1])

def reference(starting_stream, multiplier_matrix, memory_path_matrix, filter_coefficients, memory_valve_matrix, entry_valve_matrix, forgetting_parameters, timestep_forgetting_multiplier, spike_extra, exit_projector_matrix, prelude_rms_gains, finishing_rms_gains):
    stream = starting_stream
    full_width = memory_path_matrix.shape[2]
    per_block = full_width // N_TP
    for tier_number in range(LAYERS):
        floats = stream.astype(jnp.float32)
        normed = norm_rows(floats, prelude_rms_gains[tier_number]).astype(jnp.bfloat16)
        branch = jnp.dot(normed, multiplier_matrix[tier_number], preferred_element_type=jnp.float32).astype(jnp.bfloat16)
        recurrent = jnp.dot(normed, memory_path_matrix[tier_number], preferred_element_type=jnp.float32).astype(jnp.bfloat16)
        padded = jnp.concatenate([jnp.zeros((CONV - 1, full_width), jnp.bfloat16), recurrent], axis=0)
        conv_sum = jnp.zeros((TOKENS, full_width), jnp.float32)
        for offset in range(CONV):
            conv_sum = conv_sum + padded[offset:offset + TOKENS].astype(jnp.float32) * filter_coefficients[tier_number, offset].astype(jnp.float32)
        convolved = conv_sum.astype(jnp.bfloat16)
        blocks = convolved.astype(jnp.float32).reshape(TOKENS, BLOCKS, BLOCK_W)
        memory_valve_amount = jax.nn.sigmoid(jnp.einsum('tnc,ncd->tnd', blocks, memory_valve_matrix[tier_number].astype(jnp.float32)).reshape(TOKENS, full_width))
        inject = jax.nn.sigmoid(jnp.einsum('tnc,ncd->tnd', blocks, entry_valve_matrix[tier_number].astype(jnp.float32)).reshape(TOKENS, full_width))
        logarithmic_persistence = -SQUASH_POWER * memory_valve_amount * jax.nn.softplus(-forgetting_parameters[tier_number])[None, :] * timestep_forgetting_multiplier[:, None] + spike_extra
        keep_rate = jnp.exp(logarithmic_persistence)
        driven = inject * convolved.astype(jnp.float32) * jnp.sqrt(-jnp.expm1(2.0 * logarithmic_persistence))
        state_seq = lax.associative_scan(combine_pairs, (keep_rate, driven), axis=0)[1]
        mixed_in = (jax.nn.gelu(branch.astype(jnp.float32)) * state_seq).astype(jnp.bfloat16)
        mixed_sum = jnp.zeros((TOKENS, D), jnp.float32)
        for block_no in range(N_TP):
            lower = block_no * per_block
            product = jnp.dot(mixed_in[:, lower:lower + per_block], exit_projector_matrix[tier_number, lower:lower + per_block], preferred_element_type=jnp.float32)
            mixed_sum = mixed_sum + lax.optimization_barrier(product.astype(jnp.bfloat16)).astype(jnp.float32)
        stream = (floats + mixed_sum).astype(jnp.bfloat16)
    return norm_rows(stream.astype(jnp.float32), finishing_rms_gains).astype(jnp.bfloat16)
```

```python
import functools

import jax
import jax.numpy as jnp
from jax import lax
from jax.experimental import pallas as pl
from jax.experimental.pallas import tpu as pltpu
from jax.sharding import PartitionSpec as P

BLOCK_W = 256


EPSILON = 1e-06
SQUASH_POWER = 8.0


def from_behind(value, axis, steps):
    count = lax.axis_size(axis)
    first, last = (max(0, -steps), min(count, count - steps))
    return lax.ppermute(value, axis, [(source, source + steps) for source in range(first, last)])


def entering(part, axis, combine, identity):
    place = lax.axis_index(axis)
    gathered = jax.tree.map(lambda a: lax.all_gather(a, axis), part)
    state = jax.tree.map(lambda a, e: jnp.zeros_like(a) + jnp.asarray(e, a.dtype), part, identity)

    def one(lap, state):
        return combine(
            state, jax.tree.map(lambda a: lax.dynamic_index_in_dim(a, lap, 0, False), gathered)
        )

    return lax.fori_loop(0, place, one, state)


def combine_pairs(earlier, later):
    return (earlier[0] * later[0], later[0] * earlier[1] + later[1])


def gather_rows(own_cols):
    return lax.all_gather(own_cols, "tp", axis=1, tiled=True)


def on_device(
    starting_stream,
    multiplier_matrix,
    memory_path_matrix,
    filter_coefficients,
    memory_valve_matrix,
    entry_valve_matrix,
    forgetting_parameters,
    timestep_forgetting_multiplier,
    spike_extra,
    exit_projector_matrix,
    prelude_rms_gains,
    finishing_rms_gains,
):
    tok_rows = starting_stream.shape[0]
    channels = memory_path_matrix.shape[2]
    own_cols = starting_stream
    full_rows = gather_rows(starting_stream)
    for tier_number in range(memory_path_matrix.shape[0]):
        floats = full_rows.astype(jnp.float32)
        mean_square = jnp.mean(floats * floats, axis=1, keepdims=True)
        normed = (
            floats * lax.rsqrt(mean_square + EPSILON) * prelude_rms_gains[tier_number][None, :]
        ).astype(jnp.bfloat16)
        branch_acc = jnp.dot(
            normed,
            lax.all_gather(multiplier_matrix[tier_number], "sp", axis=0, tiled=True),
            preferred_element_type=jnp.float32,
        )
        recur_acc = jnp.dot(
            normed,
            lax.all_gather(memory_path_matrix[tier_number], "sp", axis=0, tiled=True),
            preferred_element_type=jnp.float32,
        )
        branch = branch_acc.astype(jnp.bfloat16)
        recurrent = recur_acc.astype(jnp.bfloat16)
        taps_now = filter_coefficients[tier_number]
        reach_back = taps_now.shape[0] - 1
        halo_rows = from_behind(recurrent[tok_rows - reach_back :], "sp", 1)
        extended = jnp.concatenate([halo_rows, recurrent], axis=0)
        conv_sum = jnp.zeros((tok_rows, channels), jnp.float32)
        for offset in range(taps_now.shape[0]):
            conv_sum = conv_sum + extended[offset : offset + tok_rows].astype(
                jnp.float32
            ) * taps_now[offset].astype(jnp.float32)
        convolved = conv_sum.astype(jnp.bfloat16)
        blocks = convolved.reshape(tok_rows, channels // BLOCK_W, BLOCK_W)
        reset_gate = jax.nn.sigmoid(
            jnp.einsum(
                "tnc,ncd->tnd",
                blocks,
                memory_valve_matrix[tier_number],
                preferred_element_type=jnp.float32,
            ).reshape(tok_rows, channels)
        )
        inject = jax.nn.sigmoid(
            jnp.einsum(
                "tnc,ncd->tnd",
                blocks,
                entry_valve_matrix[tier_number],
                preferred_element_type=jnp.float32,
            ).reshape(tok_rows, channels)
        )
        logarithmic_persistence = (
            -SQUASH_POWER
            * reset_gate
            * jax.nn.softplus(-forgetting_parameters[tier_number])[None, :]
            * timestep_forgetting_multiplier[:, None]
            + spike_extra
        )
        keep_rate = jnp.exp(logarithmic_persistence)
        driven = (
            inject
            * convolved.astype(jnp.float32)
            * jnp.sqrt(-jnp.expm1(2.0 * logarithmic_persistence))
        )
        keep_cum, state_local = lax.associative_scan(combine_pairs, (keep_rate, driven), axis=0)
        identity = (jnp.ones((channels,), jnp.float32), jnp.zeros((channels,), jnp.float32))
        carried = entering((keep_cum[-1], state_local[-1]), "sp", combine_pairs, identity)
        state_seq = state_local + keep_cum * carried[1][None, :]
        mixed_in = (jax.nn.gelu(branch.astype(jnp.float32)) * state_seq).astype(jnp.bfloat16)
        partial_value = jnp.dot(
            mixed_in,
            lax.all_gather(exit_projector_matrix[tier_number], "sp", axis=1, tiled=True),
            preferred_element_type=jnp.float32,
        )
        mixed_sum = lax.psum_scatter(
            partial_value.astype(jnp.bfloat16), "tp", scatter_dimension=1, tiled=True
        ).astype(jnp.float32)
        own_cols = (own_cols.astype(jnp.float32) + mixed_sum).astype(jnp.bfloat16)
        if tier_number + 1 < memory_path_matrix.shape[0]:
            full_rows = gather_rows(own_cols)
    floats = own_cols.astype(jnp.float32)
    full_width = floats.shape[1] * lax.axis_size("tp")
    square_sum = lax.psum(jnp.sum(floats * floats, axis=1), "tp")
    inv_rms = lax.rsqrt(square_sum / full_width + EPSILON)
    return (floats * inv_rms[:, None] * finishing_rms_gains[None, :]).astype(jnp.bfloat16)


MESH = pl.DeviceIdType.MESH
F32, BF16 = jnp.float32, jnp.bfloat16


def one_minus_exp(u):
    series = -u * (
        1 + u / 2 * (1 + u / 3 * (1 + u / 4 * (1 + u / 5 * (1 + u / 6 * (1 + u / 7)))))
    )
    return jnp.where(u > -0.35, series, 1.0 - jnp.exp(u))


def shifted(value, steps, fill):
    rows = value.shape[0]
    if steps % 8 == 0:
        top = jnp.full((steps, value.shape[1]), fill, value.dtype)
        return jnp.concatenate([top, value[: rows - steps]], axis=0)
    at = lax.broadcasted_iota(jnp.int32, value.shape, 0)
    return jnp.where(at < steps, fill, pltpu.roll(value, steps, 0))


def fused(
    sizes,
    x_ref,
    branch_w,
    memory_w,
    exit_w,
    taps_ref,
    reset_w,
    inject_w,
    rate_ref,
    mult_ref,
    spike_ref,
    gains_ref,
    final_ref,
    out_ref,
    win,
    wout,
    agx,
    xs,
    nrm,
    ext,
    halo,
    keep_s,
    state_s,
    gel_s,
    mix_s,
    part,
    from_sib,
    pair,
    from_far,
    cry_out,
    cry_in,
    hacc,
    sq_out,
    sq_in,
    sem_own,
    sem_w_recv,
    sem_up,
    sem_down,
    sem_y,
    sem_ag_send,
    sem_ag_recv,
    sem_rs_send,
    sem_rs_recv,
    sem_h,
    sem_c_send,
    sem_c_recv,
    sem_q_send,
    sem_q_recv,
):
    layers, n_sp, n_tp, n_grp, rows, chans, feats, depth, pieces = sizes
    chips = n_tp // 2
    g, s, t = lax.axis_index("grp"), lax.axis_index("sp"), lax.axis_index("tp")
    core = lax.rem(t, 2)
    chip = t // 2
    sib = chip * 2 + 1 - core
    full = n_tp * feats

    def up():
        return {"sp": s + 1}

    def down():
        return {"sp": s - 1}

    def across():
        return {"grp": 1 - g}

    barrier = pltpu.get_barrier_semaphore()
    for d in range(1, n_tp):
        pl.semaphore_signal(
            barrier, inc=1, device_id={"tp": lax.rem(t + d, n_tp)}, device_id_type=MESH
        )
    for d in range(1, n_sp):
        pl.semaphore_signal(
            barrier, inc=1, device_id={"sp": lax.rem(s + d, n_sp)}, device_id_type=MESH
        )
    pl.semaphore_signal(barrier, inc=1, device_id=across(), device_id_type=MESH)
    pl.semaphore_wait(barrier, n_tp - 1 + n_sp - 1 + 1)

    def own_block(m):
        return (memory_w, branch_w, exit_w)[m % 3].at[m // 3]

    def held(m, j):
        return win.at[2 * (m // 3) + m % 3, j] if m % 3 < 2 else wout.at[m // 3, j]

    def sent(src, m, j, half, send_sem, where):
        return pltpu.make_async_remote_copy(
            src_ref=src,
            dst_ref=held(m, j).at[half],
            send_sem=send_sem.at[m, j],
            recv_sem=sem_w_recv.at[m, j, half],
            device_id=where,
            device_id_type=MESH,
        )

    def start_own(m):
        src = own_block(m).at[g]

        @pl.when(s < n_sp - 1)
        def _():
            sent(src, m, s, g, sem_up, up()).start()

        @pl.when(s > 0)
        def _():
            sent(src, m, s, g, sem_down, down()).start()

    def keep_own(m):
        return pltpu.make_async_copy(own_block(m), held(m, s), sem_own.at[m])

    def pump(m):
        for d in range(1, n_sp):

            @pl.when(s - d >= 0)
            def _():
                j = s - d
                src = held(m, j).at[g]
                sent(src, m, j, g, sem_up, up()).wait_recv()

                @pl.when(s < n_sp - 1)
                def _():
                    sent(src, m, j, g, sem_up, up()).start()

                sent(src, m, j, g, sem_y, across()).start()

            @pl.when(s + d < n_sp)
            def _():
                j = s + d
                src = held(m, j).at[g]
                sent(src, m, j, g, sem_down, down()).wait_recv()

                @pl.when(s > 0)
                def _():
                    sent(src, m, j, g, sem_down, down()).start()

                sent(src, m, j, g, sem_y, across()).start()

        if m + 3 < 3 * layers:
            start_own(m + 3)

    def arrived(m):
        keep_own(m).wait()
        for d in range(1, n_sp):
            j = lax.rem(s + d, n_sp)
            src = held(m, j).at[1 - g]
            sent(src, m, j, 1 - g, sem_y, across()).wait_recv()

    def close_weights():
        for m in range(3 * layers):
            for j in range(n_sp):
                src = held(m, j).at[g]

                @pl.when((s < n_sp - 1) & (j <= s))
                def _():
                    sent(src, m, j, g, sem_up, up()).wait_send()

                @pl.when((s > 0) & (j >= s))
                def _():
                    sent(src, m, j, g, sem_down, down()).wait_send()

                @pl.when(j != s)
                def _():
                    sent(src, m, j, g, sem_y, across()).wait_send()

    for m in range(3 * layers):
        keep_own(m).start()

    def ag_copy(src, layer, owner, k, where):
        return pltpu.make_async_remote_copy(
            src_ref=src,
            dst_ref=agx.at[layer, owner],
            send_sem=sem_ag_send.at[layer, k],
            recv_sem=sem_ag_recv.at[layer, owner],
            device_id={"tp": where},
            device_id_type=MESH,
        )

    def ag_start(layer, src):
        for d in range(1, chips):
            ag_copy(src, layer, t, d, lax.rem(t + 2 * d, n_tp)).start()
        ag_copy(src, layer, t, 0, sib).start()

    def ag_finish(layer, src):
        for d in range(1, chips):
            owner = lax.rem(t + 2 * d, n_tp)
            block = agx.at[layer, owner]
            ag_copy(block, layer, owner, d, sib).wait_recv()
            ag_copy(block, layer, owner, chips + d, sib).start()
        ag_copy(src, layer, sib, 0, sib).wait_recv()
        for d in range(1, chips):
            owner = lax.rem(sib + 2 * d, n_tp)
            ag_copy(agx.at[layer, owner], layer, owner, d, sib).wait_recv()

    def ag_close(layer, src):
        for d in range(1, chips):
            ag_copy(src, layer, t, d, sib).wait_send()
            ag_copy(src, layer, t, chips + d, sib).wait_send()
        ag_copy(src, layer, t, 0, sib).wait_send()

    ag_start(0, x_ref)
    for m in range(min(3, 3 * layers)):
        start_own(m)

    step = rows // pieces

    def normalize(layer):
        def one(i, carry):
            at = pl.ds(pl.multiple_of(i * step, step), step)
            total = jnp.zeros((step, 1), F32)
            for p in range(n_tp):
                f = agx[layer, p, at].astype(F32)
                total = total + jnp.sum(f * f, axis=1, keepdims=True)
            inv = lax.rsqrt(total / full + EPSILON)
            for p in range(n_tp):
                cols = slice(p * feats, (p + 1) * feats)
                f = agx[layer, p, at].astype(F32)
                gain = gains_ref[layer : layer + 1, cols]
                nrm[at, cols] = (f * inv * gain).astype(BF16)
            return carry

        lax.fori_loop(0, pieces, one, 0)

    def project(idx):
        total = None
        for j in range(n_sp):
            term = jnp.dot(
                nrm[:, j * depth : (j + 1) * depth],
                win[idx, j].reshape(depth, chans),
                preferred_element_type=F32,
            )
            total = term if total is None else total + term
        return total.astype(BF16).astype(F32)

    def halo_copy(layer):
        return pltpu.make_async_remote_copy(
            src_ref=ext.at[layer, pl.ds(rows, 8)],
            dst_ref=halo.at[layer],
            send_sem=sem_h.at[layer, 0],
            recv_sem=sem_h.at[layer, 1],
            device_id=up(),
            device_id_type=MESH,
        )

    def carry_copy(layer, d):
        return pltpu.make_async_remote_copy(
            src_ref=cry_out.at[layer],
            dst_ref=cry_in.at[layer, s],
            send_sem=sem_c_send.at[layer, d],
            recv_sem=sem_c_recv.at[layer, s],
            device_id={"sp": s + d},
            device_id_type=MESH,
        )

    def carry_wait(layer, j):
        pltpu.make_async_remote_copy(
            src_ref=cry_out.at[layer],
            dst_ref=cry_in.at[layer, j],
            send_sem=sem_c_send.at[layer, 0],
            recv_sem=sem_c_recv.at[layer, j],
            device_id={"sp": s},
            device_id_type=MESH,
        ).wait_recv()

    def rs_copy(src, dst, layer, k, where):
        return pltpu.make_async_remote_copy(
            src_ref=src,
            dst_ref=dst,
            send_sem=sem_rs_send.at[layer, k],
            recv_sem=sem_rs_recv.at[layer, k],
            device_id={"tp": where},
            device_id_type=MESH,
        )

    def near_copy(layer, q):
        to = lax.rem(sib + 2 * q, n_tp)
        return rs_copy(part.at[layer, to], from_sib.at[layer, q], layer, q, sib)

    def far_copy(layer, q):
        where = lax.rem(t + 2 * q, n_tp)
        return rs_copy(pair.at[layer, q], from_far.at[layer, q], layer, chips + q, where)

    for layer in range(layers):
        m0 = 3 * layer
        src = x_ref if layer == 0 else xs.at[layer]
        agx[layer, t] = src[...]
        ag_finish(layer, src)
        normalize(layer)
        pump(m0)
        arrived(m0)
        ext[layer, 8:] = project(2 * layer)

        @pl.when(s < n_sp - 1)
        def _():
            halo_copy(layer).start()

        @pl.when(s == 0)
        def _():
            halo[layer] = jnp.zeros((8, chans), F32)

        @pl.when(s > 0)
        def _():
            halo_copy(layer).wait_recv()

        ext[layer, :8] = halo[layer]
        n_taps = taps_ref.shape[1]
        base = 8 - (n_taps - 1)
        for b in range(chans // BLOCK_W):
            cols = slice(b * BLOCK_W, (b + 1) * BLOCK_W)
            conv = jnp.zeros((rows, BLOCK_W), F32)
            for k in range(n_taps):
                tap = taps_ref[layer, k : k + 1, cols].astype(F32)
                conv = conv + ext[layer, base + k : base + k + rows, cols] * tap
            conv = conv.astype(BF16)
            reset = jax.nn.sigmoid(
                jnp.dot(conv, reset_w[layer, b], preferred_element_type=F32)
            )
            inject = jax.nn.sigmoid(
                jnp.dot(conv, inject_w[layer, b], preferred_element_type=F32)
            )
            log_keep = (
                reset * rate_ref[layer : layer + 1, cols] * mult_ref[...]
                + spike_ref[:, cols]
            )
            keep = jnp.exp(log_keep)
            state = inject * conv.astype(F32) * jnp.sqrt(one_minus_exp(2.0 * log_keep))
            lag = 1
            while lag < rows:
                state = keep * shifted(state, lag, 0.0) + state
                keep = keep * shifted(keep, lag, 1.0)
                lag *= 2
            keep_s[:, cols] = keep
            state_s[:, cols] = state
            cry_out[layer, 0:1, cols] = keep[rows - 1 :]
            cry_out[layer, 1:2, cols] = state[rows - 1 :]
        for d in range(1, n_sp):

            @pl.when(s + d < n_sp)
            def _():
                carry_copy(layer, d).start()

        pump(m0 + 1)
        arrived(m0 + 1)
        gel_s[...] = jax.nn.gelu(project(2 * layer + 1))
        hacc[...] = jnp.zeros((1, chans), F32)
        for j in range(n_sp - 1):

            @pl.when(j < s)
            def _():
                carry_wait(layer, j)
                hacc[...] = cry_in[layer, j, 0:1] * hacc[...] + cry_in[layer, j, 1:2]

        mix_s[...] = (
            gel_s[...] * (state_s[...] + keep_s[...] * hacc[...])
        ).astype(BF16)
        pump(m0 + 2)
        arrived(m0 + 2)
        unit = min(depth, feats)
        for j in range(n_sp):
            done = jnp.dot(
                mix_s[...],
                wout[layer, j].reshape(chans, depth),
                preferred_element_type=F32,
            ).astype(BF16)
            for c in range(0, depth, unit):
                at = j * depth + c
                low = at % feats
                part[layer, at // feats, :, low : low + unit] = done[:, c : c + unit]
        for q in list(range(1, chips)) + [0]:
            near_copy(layer, q).start()
        for q in range(1, chips):
            near_copy(layer, q).wait_recv()
            to = lax.rem(t + 2 * q, n_tp)
            pair[layer, q] = (
                part[layer, to].astype(F32) + from_sib[layer, q].astype(F32)
            ).astype(BF16)
            far_copy(layer, q).start()
        near_copy(layer, 0).wait_recv()
        mixed = part[layer, t].astype(F32) + from_sib[layer, 0].astype(F32)
        for q in range(1, chips):
            far_copy(layer, q).wait_recv()
            mixed = mixed + from_far[layer, q].astype(F32)
        fresh = (src[...].astype(F32) + mixed).astype(BF16)
        xs[layer + 1] = fresh
        if layer + 1 < layers:
            ag_start(layer + 1, xs.at[layer + 1])

    last = xs[layers].astype(F32)
    square = jnp.sum(last * last, axis=1, keepdims=True)
    sq_out[...] = jnp.broadcast_to(square, (rows, 128)).T[0:8]

    def sq_copy(d):
        return pltpu.make_async_remote_copy(
            src_ref=sq_out,
            dst_ref=sq_in.at[d],
            send_sem=sem_q_send.at[d],
            recv_sem=sem_q_recv.at[d],
            device_id={"tp": lax.rem(t + d, n_tp)},
            device_id_type=MESH,
        )

    for d in range(1, n_tp):
        sq_copy(d).start()
    total = sq_out[0:1]
    for d in range(1, n_tp):
        sq_copy(d).wait_recv()
        total = total + sq_in[d, 0:1]
    inv = lax.rsqrt(total / full + EPSILON)
    inv = jnp.broadcast_to(inv, (128, rows)).T[:, 0:1]
    out_ref[...] = (xs[layers].astype(F32) * inv * final_ref[...]).astype(BF16)

    close_weights()
    for layer in range(layers):
        ag_close(layer, x_ref if layer == 0 else xs.at[layer])

        @pl.when(s < n_sp - 1)
        def _():
            halo_copy(layer).wait_send()

        for d in range(1, n_sp):

            @pl.when(s + d < n_sp)
            def _():
                carry_copy(layer, d).wait_send()

        for q in range(chips):
            near_copy(layer, q).wait_send()
        for q in range(1, chips):
            far_copy(layer, q).wait_send()
    for d in range(1, n_tp):
        sq_copy(d).wait_send()


def in_one_kernel(
    sizes_of,
    starting_stream,
    multiplier_matrix,
    memory_path_matrix,
    filter_coefficients,
    memory_valve_matrix,
    entry_valve_matrix,
    forgetting_parameters,
    timestep_forgetting_multiplier,
    spike_extra,
    exit_projector_matrix,
    prelude_rms_gains,
    finishing_rms_gains,
):
    n_grp, n_sp, n_tp = sizes_of
    rows, feats = starting_stream.shape
    layers, depth, chans = memory_path_matrix.shape
    pieces = rows // 128 if rows % 128 == 0 else 1
    sizes = (layers, n_sp, n_tp, n_grp, rows, chans, feats, depth, pieces)
    chips = n_tp // 2
    half_in = (layers, 2, depth // 2, chans)
    half_out = (layers, 2, chans // 2, depth)
    rate = -SQUASH_POWER * jax.nn.softplus(-forgetting_parameters)
    vmem = pl.BlockSpec(memory_space=pltpu.VMEM)
    hbm = pl.BlockSpec(memory_space=pl.ANY)
    count = 3 * layers
    dma = pltpu.SemaphoreType.DMA
    return pl.pallas_call(
        functools.partial(fused, sizes),
        out_shape=jax.ShapeDtypeStruct((rows, feats), BF16),
        in_specs=[vmem, hbm, hbm, hbm] + [vmem] * 8,
        out_specs=vmem,
        scratch_shapes=[
            pltpu.VMEM((2 * layers, n_sp, 2, depth // 2, chans), BF16),
            pltpu.VMEM((layers, n_sp, 2, chans // 2, depth), BF16),
            pltpu.VMEM((layers, n_tp, rows, feats), BF16),
            pltpu.VMEM((layers + 1, rows, feats), BF16),
            pltpu.VMEM((rows, n_tp * feats), BF16),
            pltpu.VMEM((layers, 8 + rows, chans), F32),
            pltpu.VMEM((layers, 8, chans), F32),
            pltpu.VMEM((rows, chans), F32),
            pltpu.VMEM((rows, chans), F32),
            pltpu.VMEM((rows, chans), F32),
            pltpu.VMEM((rows, chans), BF16),
            pltpu.VMEM((layers, n_tp, rows, feats), BF16),
            pltpu.VMEM((layers, chips, rows, feats), BF16),
            pltpu.VMEM((layers, chips, rows, feats), BF16),
            pltpu.VMEM((layers, chips, rows, feats), BF16),
            pltpu.VMEM((layers, 2, chans), F32),
            pltpu.VMEM((layers, n_sp, 2, chans), F32),
            pltpu.VMEM((1, chans), F32),
            pltpu.VMEM((8, rows), F32),
            pltpu.VMEM((n_tp, 8, rows), F32),
            dma((count,)),
            dma((count, n_sp, 2)),
            dma((count, n_sp)),
            dma((count, n_sp)),
            dma((count, n_sp)),
            dma((layers, 2 * chips)),
            dma((layers, n_tp)),
            dma((layers, 2 * chips)),
            dma((layers, 2 * chips)),
            dma((layers, 2)),
            dma((layers, n_sp)),
            dma((layers, n_sp)),
            dma((n_tp,)),
            dma((n_tp,)),
        ],
        compiler_params=pltpu.CompilerParams(
            collective_id=0, has_side_effects=True, vmem_limit_bytes=60 * 2**20
        ),
    )(
        starting_stream,
        multiplier_matrix.reshape(half_in),
        memory_path_matrix.reshape(half_in),
        exit_projector_matrix.reshape(half_out),
        filter_coefficients,
        memory_valve_matrix,
        entry_valve_matrix,
        rate,
        timestep_forgetting_multiplier.reshape(rows, 1),
        spike_extra,
        prelude_rms_gains,
        finishing_rms_gains.reshape(1, feats),
    )


def on_each(sizes_of, *arrays):
    stream, memory = arrays[0], arrays[2]
    n_grp, n_sp, n_tp = sizes_of
    rows, feats = stream.shape
    depth, chans = memory.shape[1:]
    unit = min(depth, feats)
    fits = (
        n_grp == 2
        and n_sp > 1
        and n_tp % 2 == 0
        and rows % 128 == 0
        and depth % 128 == 0
        and feats % 128 == 0
        and chans % BLOCK_W == 0
        and depth % unit == 0
        and feats % unit == 0
    )
    if fits:
        return in_one_kernel(sizes_of, *arrays)
    return on_device(*arrays)


def solution(mesh):
    sizes_of = tuple(mesh.shape[axis] for axis in ("grp", "sp", "tp"))
    body = functools.partial(on_each, sizes_of)
    return jax.shard_map(
        body,
        mesh=mesh,
        in_specs=(
            P(("grp", "sp"), "tp"),
            P(None, "sp", "tp"),
            P(None, "sp", "tp"),
            P(None, None, "tp"),
            P(None, "tp", None, None),
            P(None, "tp", None, None),
            P(None, "tp"),
            P(("grp", "sp")),
            P(("grp", "sp"), "tp"),
            P(None, "tp", "sp"),
            P(),
            P("tp"),
        ),
        out_specs=P(("grp", "sp"), "tp"),
        check_vma=False,
    )
```

```python
import functools

import jax
import jax.numpy as jnp
from jax import lax
from jax.experimental import pallas as pl
from jax.experimental.pallas import tpu as pltpu
from jax.sharding import PartitionSpec as P

BLOCK_W = 256


EPSILON = 1e-06
SQUASH_POWER = 8.0


def from_behind(value, axis, steps):
    count = lax.axis_size(axis)
    first, last = (max(0, -steps), min(count, count - steps))
    return lax.ppermute(value, axis, [(source, source + steps) for source in range(first, last)])


def entering(part, axis, combine, identity):
    place = lax.axis_index(axis)
    gathered = jax.tree.map(lambda a: lax.all_gather(a, axis), part)
    state = jax.tree.map(lambda a, e: jnp.zeros_like(a) + jnp.asarray(e, a.dtype), part, identity)

    def one(lap, state):
        return combine(
            state, jax.tree.map(lambda a: lax.dynamic_index_in_dim(a, lap, 0, False), gathered)
        )

    return lax.fori_loop(0, place, one, state)


def combine_pairs(earlier, later):
    return (earlier[0] * later[0], later[0] * earlier[1] + later[1])


def gather_rows(own_cols):
    return lax.all_gather(own_cols, "tp", axis=1, tiled=True)


def on_device(
    starting_stream,
    multiplier_matrix,
    memory_path_matrix,
    filter_coefficients,
    memory_valve_matrix,
    entry_valve_matrix,
    forgetting_parameters,
    timestep_forgetting_multiplier,
    spike_extra,
    exit_projector_matrix,
    prelude_rms_gains,
    finishing_rms_gains,
):
    tok_rows = starting_stream.shape[0]
    channels = memory_path_matrix.shape[2]
    own_cols = starting_stream
    full_rows = gather_rows(starting_stream)
    for tier_number in range(memory_path_matrix.shape[0]):
        floats = full_rows.astype(jnp.float32)
        mean_square = jnp.mean(floats * floats, axis=1, keepdims=True)
        normed = (
            floats * lax.rsqrt(mean_square + EPSILON) * prelude_rms_gains[tier_number][None, :]
        ).astype(jnp.bfloat16)
        branch_acc = jnp.dot(
            normed,
            lax.all_gather(multiplier_matrix[tier_number], "sp", axis=0, tiled=True),
            preferred_element_type=jnp.float32,
        )
        recur_acc = jnp.dot(
            normed,
            lax.all_gather(memory_path_matrix[tier_number], "sp", axis=0, tiled=True),
            preferred_element_type=jnp.float32,
        )
        branch = branch_acc.astype(jnp.bfloat16)
        recurrent = recur_acc.astype(jnp.bfloat16)
        taps_now = filter_coefficients[tier_number]
        reach_back = taps_now.shape[0] - 1
        halo_rows = from_behind(recurrent[tok_rows - reach_back :], "sp", 1)
        extended = jnp.concatenate([halo_rows, recurrent], axis=0)
        conv_sum = jnp.zeros((tok_rows, channels), jnp.float32)
        for offset in range(taps_now.shape[0]):
            conv_sum = conv_sum + extended[offset : offset + tok_rows].astype(
                jnp.float32
            ) * taps_now[offset].astype(jnp.float32)
        convolved = conv_sum.astype(jnp.bfloat16)
        blocks = convolved.reshape(tok_rows, channels // BLOCK_W, BLOCK_W)
        reset_gate = jax.nn.sigmoid(
            jnp.einsum(
                "tnc,ncd->tnd",
                blocks,
                memory_valve_matrix[tier_number],
                preferred_element_type=jnp.float32,
            ).reshape(tok_rows, channels)
        )
        inject = jax.nn.sigmoid(
            jnp.einsum(
                "tnc,ncd->tnd",
                blocks,
                entry_valve_matrix[tier_number],
                preferred_element_type=jnp.float32,
            ).reshape(tok_rows, channels)
        )
        logarithmic_persistence = (
            -SQUASH_POWER
            * reset_gate
            * jax.nn.softplus(-forgetting_parameters[tier_number])[None, :]
            * timestep_forgetting_multiplier[:, None]
            + spike_extra
        )
        keep_rate = jnp.exp(logarithmic_persistence)
        driven = (
            inject
            * convolved.astype(jnp.float32)
            * jnp.sqrt(-jnp.expm1(2.0 * logarithmic_persistence))
        )
        keep_cum, state_local = lax.associative_scan(combine_pairs, (keep_rate, driven), axis=0)
        identity = (jnp.ones((channels,), jnp.float32), jnp.zeros((channels,), jnp.float32))
        carried = entering((keep_cum[-1], state_local[-1]), "sp", combine_pairs, identity)
        state_seq = state_local + keep_cum * carried[1][None, :]
        mixed_in = (jax.nn.gelu(branch.astype(jnp.float32)) * state_seq).astype(jnp.bfloat16)
        partial_value = jnp.dot(
            mixed_in,
            lax.all_gather(exit_projector_matrix[tier_number], "sp", axis=1, tiled=True),
            preferred_element_type=jnp.float32,
        )
        mixed_sum = lax.psum_scatter(
            partial_value.astype(jnp.bfloat16), "tp", scatter_dimension=1, tiled=True
        ).astype(jnp.float32)
        own_cols = (own_cols.astype(jnp.float32) + mixed_sum).astype(jnp.bfloat16)
        if tier_number + 1 < memory_path_matrix.shape[0]:
            full_rows = gather_rows(own_cols)
    floats = own_cols.astype(jnp.float32)
    full_width = floats.shape[1] * lax.axis_size("tp")
    square_sum = lax.psum(jnp.sum(floats * floats, axis=1), "tp")
    inv_rms = lax.rsqrt(square_sum / full_width + EPSILON)
    return (floats * inv_rms[:, None] * finishing_rms_gains[None, :]).astype(jnp.bfloat16)


MESH = pl.DeviceIdType.MESH
F32, BF16 = jnp.float32, jnp.bfloat16


def one_minus_exp(u):
    series = -u * (
        1 + u / 2 * (1 + u / 3 * (1 + u / 4 * (1 + u / 5 * (1 + u / 6 * (1 + u / 7)))))
    )
    return jnp.where(u > -0.35, series, 1.0 - jnp.exp(u))


def shifted(value, steps, fill):
    rows = value.shape[0]
    if steps % 8 == 0:
        top = jnp.full((steps, value.shape[1]), fill, value.dtype)
        return jnp.concatenate([top, value[: rows - steps]], axis=0)
    at = lax.broadcasted_iota(jnp.int32, value.shape, 0)
    return jnp.where(at < steps, fill, pltpu.roll(value, steps, 0))


def fused(
    sizes,
    x_ref,
    branch_w,
    memory_w,
    exit_w,
    taps_ref,
    reset_w,
    inject_w,
    rate_ref,
    mult_ref,
    spike_ref,
    gains_ref,
    final_ref,
    out_ref,
    win,
    wout,
    agx,
    xs,
    nrm,
    ext,
    halo,
    keep_s,
    state_s,
    gel_s,
    mix_s,
    part,
    from_sib,
    pair,
    from_far,
    cry_out,
    cry_in,
    hacc,
    sq_out,
    sq_in,
    sem_own,
    sem_w_recv,
    sem_up,
    sem_down,
    sem_y,
    sem_ag_send,
    sem_ag_recv,
    sem_rs_send,
    sem_rs_recv,
    sem_h,
    sem_c_send,
    sem_c_recv,
    sem_q_send,
    sem_q_recv,
):
    layers, n_sp, n_tp, n_grp, rows, chans, feats, depth, pieces = sizes
    chips = n_tp // 2
    g, s, t = lax.axis_index("grp"), lax.axis_index("sp"), lax.axis_index("tp")
    core = lax.rem(t, 2)
    chip = t // 2
    sib = chip * 2 + 1 - core
    full = n_tp * feats

    def up():
        return {"sp": s + 1}

    def down():
        return {"sp": s - 1}

    def across():
        return {"grp": 1 - g}

    barrier = pltpu.get_barrier_semaphore()
    for d in range(1, n_tp):
        pl.semaphore_signal(
            barrier, inc=1, device_id={"tp": lax.rem(t + d, n_tp)}, device_id_type=MESH
        )
    for d in range(1, n_sp):
        pl.semaphore_signal(
            barrier, inc=1, device_id={"sp": lax.rem(s + d, n_sp)}, device_id_type=MESH
        )
    pl.semaphore_signal(barrier, inc=1, device_id=across(), device_id_type=MESH)
    pl.semaphore_wait(barrier, n_tp - 1 + n_sp - 1 + 1)

    def own_block(m):
        return (memory_w, branch_w, exit_w)[m % 3].at[m // 3]

    def held(m, j):
        return win.at[2 * (m // 3) + m % 3, j] if m % 3 < 2 else wout.at[m // 3, j]

    def sent(src, m, j, half, send_sem, where):
        return pltpu.make_async_remote_copy(
            src_ref=src,
            dst_ref=held(m, j).at[half],
            send_sem=send_sem.at[m, j],
            recv_sem=sem_w_recv.at[m, j, half],
            device_id=where,
            device_id_type=MESH,
        )

    def start_own(m):
        src = own_block(m).at[g]

        @pl.when(s < n_sp - 1)
        def _():
            sent(src, m, s, g, sem_up, up()).start()

        @pl.when(s > 0)
        def _():
            sent(src, m, s, g, sem_down, down()).start()

    def keep_own(m):
        return pltpu.make_async_copy(own_block(m), held(m, s), sem_own.at[m])

    items = [(m, d) for m in range(3 * layers) for d in range(1, n_sp)]
    place = [0]

    def pump(m, d):
        @pl.when(s - d >= 0)
        def _():
            j = s - d
            src = held(m, j).at[g]
            sent(src, m, j, g, sem_up, up()).wait_recv()

            @pl.when(s < n_sp - 1)
            def _():
                sent(src, m, j, g, sem_up, up()).start()

            sent(src, m, j, g, sem_y, across()).start()

        @pl.when(s + d < n_sp)
        def _():
            j = s + d
            src = held(m, j).at[g]
            sent(src, m, j, g, sem_down, down()).wait_recv()

            @pl.when(s > 0)
            def _():
                sent(src, m, j, g, sem_down, down()).start()

            sent(src, m, j, g, sem_y, across()).start()

        if d == n_sp - 1 and m + 2 < 3 * layers:
            start_own(m + 2)

    def advance(steps):
        for m, d in items[place[0] : place[0] + steps]:
            pump(m, d)
        place[0] = min(place[0] + steps, len(items))

    def reach(m, d):
        advance(max(0, m * (n_sp - 1) + d - place[0]))

    def swapped(m, j):
        src = held(m, j).at[1 - g]
        sent(src, m, j, 1 - g, sem_y, across()).wait_recv()

    def arrived(m):
        reach(m, n_sp - 1)
        keep_own(m).wait()
        for d in range(1, n_sp):
            swapped(m, lax.rem(s + d, n_sp))

    def close_weights():
        for m in range(3 * layers):
            for j in range(n_sp):
                src = held(m, j).at[g]

                @pl.when((s < n_sp - 1) & (j <= s))
                def _():
                    sent(src, m, j, g, sem_up, up()).wait_send()

                @pl.when((s > 0) & (j >= s))
                def _():
                    sent(src, m, j, g, sem_down, down()).wait_send()

                @pl.when(j != s)
                def _():
                    sent(src, m, j, g, sem_y, across()).wait_send()

    for m in range(3 * layers):
        keep_own(m).start()

    def ag_copy(src, layer, owner, k, where):
        return pltpu.make_async_remote_copy(
            src_ref=src,
            dst_ref=agx.at[layer, owner],
            send_sem=sem_ag_send.at[layer, k],
            recv_sem=sem_ag_recv.at[layer, owner],
            device_id={"tp": where},
            device_id_type=MESH,
        )

    def ag_start(layer, src):
        for d in range(1, chips):
            ag_copy(src, layer, t, d, lax.rem(t + 2 * d, n_tp)).start()
        ag_copy(src, layer, t, 0, sib).start()

    def ag_finish(layer, src):
        for d in range(1, chips):
            owner = lax.rem(t + 2 * d, n_tp)
            block = agx.at[layer, owner]
            ag_copy(block, layer, owner, d, sib).wait_recv()
            ag_copy(block, layer, owner, chips + d, sib).start()
        ag_copy(src, layer, sib, 0, sib).wait_recv()
        for d in range(1, chips):
            owner = lax.rem(sib + 2 * d, n_tp)
            ag_copy(agx.at[layer, owner], layer, owner, d, sib).wait_recv()

    def ag_close(layer, src):
        for d in range(1, chips):
            ag_copy(src, layer, t, d, sib).wait_send()
            ag_copy(src, layer, t, chips + d, sib).wait_send()
        ag_copy(src, layer, t, 0, sib).wait_send()

    ag_start(0, x_ref)
    for m in range(2):
        start_own(m)

    step = rows // pieces

    def normalize(layer):
        def one(i, carry):
            at = pl.ds(pl.multiple_of(i * step, step), step)
            total = jnp.zeros((step, 1), F32)
            for p in range(n_tp):
                f = agx[layer, p, at].astype(F32)
                total = total + jnp.sum(f * f, axis=1, keepdims=True)
            inv = lax.rsqrt(total / full + EPSILON)
            for p in range(n_tp):
                cols = slice(p * feats, (p + 1) * feats)
                f = agx[layer, p, at].astype(F32)
                gain = gains_ref[layer : layer + 1, cols]
                nrm[at, cols] = (f * inv * gain).astype(BF16)
            return carry

        lax.fori_loop(0, pieces, one, 0)

    def project(idx):
        total = None
        for j in range(n_sp):
            term = jnp.dot(
                nrm[:, j * depth : (j + 1) * depth],
                win[idx, j].reshape(depth, chans),
                preferred_element_type=F32,
            )
            total = term if total is None else total + term
        return total.astype(BF16).astype(F32)

    def halo_copy(layer):
        return pltpu.make_async_remote_copy(
            src_ref=ext.at[layer, pl.ds(rows, 8)],
            dst_ref=halo.at[layer],
            send_sem=sem_h.at[layer, 0],
            recv_sem=sem_h.at[layer, 1],
            device_id=up(),
            device_id_type=MESH,
        )

    def carry_copy(layer, d):
        return pltpu.make_async_remote_copy(
            src_ref=cry_out.at[layer],
            dst_ref=cry_in.at[layer, s],
            send_sem=sem_c_send.at[layer, d],
            recv_sem=sem_c_recv.at[layer, s],
            device_id={"sp": s + d},
            device_id_type=MESH,
        )

    def carry_wait(layer, j):
        pltpu.make_async_remote_copy(
            src_ref=cry_out.at[layer],
            dst_ref=cry_in.at[layer, j],
            send_sem=sem_c_send.at[layer, 0],
            recv_sem=sem_c_recv.at[layer, j],
            device_id={"sp": s},
            device_id_type=MESH,
        ).wait_recv()

    def rs_copy(src, dst, layer, k, where):
        return pltpu.make_async_remote_copy(
            src_ref=src,
            dst_ref=dst,
            send_sem=sem_rs_send.at[layer, k],
            recv_sem=sem_rs_recv.at[layer, k],
            device_id={"tp": where},
            device_id_type=MESH,
        )

    def near_copy(layer, q):
        to = lax.rem(sib + 2 * q, n_tp)
        return rs_copy(part.at[layer, to], from_sib.at[layer, q], layer, q, sib)

    def far_copy(layer, q):
        where = lax.rem(t + 2 * q, n_tp)
        return rs_copy(pair.at[layer, q], from_far.at[layer, q], layer, chips + q, where)

    for layer in range(layers):
        m0 = 3 * layer
        src = x_ref if layer == 0 else xs.at[layer]
        agx[layer, t] = src[...]
        advance(1)
        ag_finish(layer, src)
        advance(1)
        normalize(layer)
        reach(m0, n_sp)
        arrived(m0)
        ext[layer, 8:] = project(2 * layer)

        @pl.when(s < n_sp - 1)
        def _():
            halo_copy(layer).start()

        advance(1)

        @pl.when(s == 0)
        def _():
            halo[layer] = jnp.zeros((8, chans), F32)

        @pl.when(s > 0)
        def _():
            halo_copy(layer).wait_recv()

        ext[layer, :8] = halo[layer]
        n_taps = taps_ref.shape[1]
        base = 8 - (n_taps - 1)
        for b in range(chans // BLOCK_W):
            cols = slice(b * BLOCK_W, (b + 1) * BLOCK_W)
            conv = jnp.zeros((rows, BLOCK_W), F32)
            for k in range(n_taps):
                tap = taps_ref[layer, k : k + 1, cols].astype(F32)
                conv = conv + ext[layer, base + k : base + k + rows, cols] * tap
            conv = conv.astype(BF16)
            reset = jax.nn.sigmoid(
                jnp.dot(conv, reset_w[layer, b], preferred_element_type=F32)
            )
            inject = jax.nn.sigmoid(
                jnp.dot(conv, inject_w[layer, b], preferred_element_type=F32)
            )
            log_keep = (
                reset * rate_ref[layer : layer + 1, cols] * mult_ref[...]
                + spike_ref[:, cols]
            )
            keep = jnp.exp(log_keep)
            state = inject * conv.astype(F32) * jnp.sqrt(one_minus_exp(2.0 * log_keep))
            lag = 1
            while lag < rows:
                state = keep * shifted(state, lag, 0.0) + state
                keep = keep * shifted(keep, lag, 1.0)
                lag *= 2
            keep_s[:, cols] = keep
            state_s[:, cols] = state
            cry_out[layer, 0:1, cols] = keep[rows - 1 :]
            cry_out[layer, 1:2, cols] = state[rows - 1 :]
            advance(1)
        for d in range(1, n_sp):

            @pl.when(s + d < n_sp)
            def _():
                carry_copy(layer, d).start()

        reach(m0 + 2, min(2, n_sp - 1))
        arrived(m0 + 1)
        gel_s[...] = jax.nn.gelu(project(2 * layer + 1))
        hacc[...] = jnp.zeros((1, chans), F32)
        for j in range(n_sp - 1):

            @pl.when(j < s)
            def _():
                carry_wait(layer, j)
                hacc[...] = cry_in[layer, j, 0:1] * hacc[...] + cry_in[layer, j, 1:2]

        mix_s[...] = (
            gel_s[...] * (state_s[...] + keep_s[...] * hacc[...])
        ).astype(BF16)
        def chips_on(j):
            return lax.rem(j // 2 - chip + chips, chips)

        def product(j):
            part[layer, j] = jnp.dot(
                mix_s[...],
                wout[layer, j].reshape(chans, depth),
                preferred_element_type=F32,
            ).astype(BF16)

            @pl.when(lax.rem(j, 2) != core)
            def _():
                near_copy(layer, chips_on(j)).start()

        def pass_on(j):
            q = chips_on(j)

            @pl.when((lax.rem(j, 2) == core) & (q != 0))
            def _():
                near_copy(layer, q).wait_recv()
                pair[layer, q] = (
                    part[layer, j].astype(F32) + from_sib[layer, q].astype(F32)
                ).astype(BF16)
                far_copy(layer, q).start()

        m = m0 + 2
        keep_own(m).wait()
        product(s)
        for d in range(1, n_sp):
            reach(m, d)
            if d > 1:
                advance(1)

            @pl.when(s - d >= 0)
            def _():
                swapped(m, s - d)
                product(s - d)

            @pl.when(s + d < n_sp)
            def _():
                swapped(m, s + d)
                product(s + d)

            if d == 1:
                pass_on(s)
            else:
                for j in (s - d + 1, s + d - 1):

                    @pl.when((j >= 0) & (j < n_sp))
                    def _():
                        pass_on(j)

        for j in (s - n_sp + 1, s + n_sp - 1):

            @pl.when((j >= 0) & (j < n_sp))
            def _():
                pass_on(j)

        advance(1)
        near_copy(layer, 0).wait_recv()
        mixed = part[layer, t].astype(F32) + from_sib[layer, 0].astype(F32)
        for q in range(1, chips):
            far_copy(layer, q).wait_recv()
            mixed = mixed + from_far[layer, q].astype(F32)
        fresh = (src[...].astype(F32) + mixed).astype(BF16)
        xs[layer + 1] = fresh
        if layer + 1 < layers:
            ag_start(layer + 1, xs.at[layer + 1])

    last = xs[layers].astype(F32)
    square = jnp.sum(last * last, axis=1, keepdims=True)
    sq_out[...] = jnp.broadcast_to(square, (rows, 128)).T[0:8]

    def sq_copy(d):
        return pltpu.make_async_remote_copy(
            src_ref=sq_out,
            dst_ref=sq_in.at[d],
            send_sem=sem_q_send.at[d],
            recv_sem=sem_q_recv.at[d],
            device_id={"tp": lax.rem(t + d, n_tp)},
            device_id_type=MESH,
        )

    for d in range(1, n_tp):
        sq_copy(d).start()
    total = sq_out[0:1]
    for d in range(1, n_tp):
        sq_copy(d).wait_recv()
        total = total + sq_in[d, 0:1]
    inv = lax.rsqrt(total / full + EPSILON)
    inv = jnp.broadcast_to(inv, (128, rows)).T[:, 0:1]
    out_ref[...] = (xs[layers].astype(F32) * inv * final_ref[...]).astype(BF16)

    close_weights()
    for layer in range(layers):
        ag_close(layer, x_ref if layer == 0 else xs.at[layer])

        @pl.when(s < n_sp - 1)
        def _():
            halo_copy(layer).wait_send()

        for d in range(1, n_sp):

            @pl.when(s + d < n_sp)
            def _():
                carry_copy(layer, d).wait_send()

        for q in range(chips):
            near_copy(layer, q).wait_send()
        for q in range(1, chips):
            far_copy(layer, q).wait_send()
    for d in range(1, n_tp):
        sq_copy(d).wait_send()


def in_one_kernel(
    sizes_of,
    starting_stream,
    multiplier_matrix,
    memory_path_matrix,
    filter_coefficients,
    memory_valve_matrix,
    entry_valve_matrix,
    forgetting_parameters,
    timestep_forgetting_multiplier,
    spike_extra,
    exit_projector_matrix,
    prelude_rms_gains,
    finishing_rms_gains,
):
    n_grp, n_sp, n_tp = sizes_of
    rows, feats = starting_stream.shape
    layers, depth, chans = memory_path_matrix.shape
    pieces = rows // 128 if rows % 128 == 0 else 1
    sizes = (layers, n_sp, n_tp, n_grp, rows, chans, feats, depth, pieces)
    chips = n_tp // 2
    half_in = (layers, 2, depth // 2, chans)
    half_out = (layers, 2, chans // 2, depth)
    rate = -SQUASH_POWER * jax.nn.softplus(-forgetting_parameters)
    vmem = pl.BlockSpec(memory_space=pltpu.VMEM)
    hbm = pl.BlockSpec(memory_space=pl.ANY)
    count = 3 * layers
    dma = pltpu.SemaphoreType.DMA
    return pl.pallas_call(
        functools.partial(fused, sizes),
        out_shape=jax.ShapeDtypeStruct((rows, feats), BF16),
        in_specs=[vmem, hbm, hbm, hbm] + [vmem] * 8,
        out_specs=vmem,
        scratch_shapes=[
            pltpu.VMEM((2 * layers, n_sp, 2, depth // 2, chans), BF16),
            pltpu.VMEM((layers, n_sp, 2, chans // 2, depth), BF16),
            pltpu.VMEM((layers, n_tp, rows, feats), BF16),
            pltpu.VMEM((layers + 1, rows, feats), BF16),
            pltpu.VMEM((rows, n_tp * feats), BF16),
            pltpu.VMEM((layers, 8 + rows, chans), F32),
            pltpu.VMEM((layers, 8, chans), F32),
            pltpu.VMEM((rows, chans), F32),
            pltpu.VMEM((rows, chans), F32),
            pltpu.VMEM((rows, chans), F32),
            pltpu.VMEM((rows, chans), BF16),
            pltpu.VMEM((layers, n_tp, rows, feats), BF16),
            pltpu.VMEM((layers, chips, rows, feats), BF16),
            pltpu.VMEM((layers, chips, rows, feats), BF16),
            pltpu.VMEM((layers, chips, rows, feats), BF16),
            pltpu.VMEM((layers, 2, chans), F32),
            pltpu.VMEM((layers, n_sp, 2, chans), F32),
            pltpu.VMEM((1, chans), F32),
            pltpu.VMEM((8, rows), F32),
            pltpu.VMEM((n_tp, 8, rows), F32),
            dma((count,)),
            dma((count, n_sp, 2)),
            dma((count, n_sp)),
            dma((count, n_sp)),
            dma((count, n_sp)),
            dma((layers, 2 * chips)),
            dma((layers, n_tp)),
            dma((layers, 2 * chips)),
            dma((layers, 2 * chips)),
            dma((layers, 2)),
            dma((layers, n_sp)),
            dma((layers, n_sp)),
            dma((n_tp,)),
            dma((n_tp,)),
        ],
        compiler_params=pltpu.CompilerParams(
            collective_id=0, has_side_effects=True, vmem_limit_bytes=60 * 2**20
        ),
    )(
        starting_stream,
        multiplier_matrix.reshape(half_in),
        memory_path_matrix.reshape(half_in),
        exit_projector_matrix.reshape(half_out),
        filter_coefficients,
        memory_valve_matrix,
        entry_valve_matrix,
        rate,
        timestep_forgetting_multiplier.reshape(rows, 1),
        spike_extra,
        prelude_rms_gains,
        finishing_rms_gains.reshape(1, feats),
    )


def on_each(sizes_of, *arrays):
    stream, memory = arrays[0], arrays[2]
    n_grp, n_sp, n_tp = sizes_of
    rows, feats = stream.shape
    depth, chans = memory.shape[1:]
    fits = (
        n_grp == 2
        and n_sp > 1
        and n_tp % 2 == 0
        and rows % 128 == 0
        and depth % 128 == 0
        and feats % 128 == 0
        and chans % BLOCK_W == 0
        and depth == feats
        and n_sp == n_tp
    )
    if fits:
        return in_one_kernel(sizes_of, *arrays)
    return on_device(*arrays)


def solution(mesh):
    sizes_of = tuple(mesh.shape[axis] for axis in ("grp", "sp", "tp"))
    body = functools.partial(on_each, sizes_of)
    return jax.shard_map(
        body,
        mesh=mesh,
        in_specs=(
            P(("grp", "sp"), "tp"),
            P(None, "sp", "tp"),
            P(None, "sp", "tp"),
            P(None, None, "tp"),
            P(None, "tp", None, None),
            P(None, "tp", None, None),
            P(None, "tp"),
            P(("grp", "sp")),
            P(("grp", "sp"), "tp"),
            P(None, "tp", "sp"),
            P(),
            P("tp"),
        ),
        out_specs=P(("grp", "sp"), "tp"),
        check_vma=False,
    )
```
